32 devices in a mesh: grp: 2 (over x), ep: 16 (over z, y, core).
Axes of the slice: x: 2, y: 2, z: 4, core: 2. Of those that a mesh axis runs over, the one named last changes fastest.
Arguments:
- tokens: bfloat16 [8192, 2048], P(('grp', 'ep')), parts along dimension 0, may hold values from -6 to 6
- norm_gain: float32 [2048], replicated, may hold values from 0.1 to 1.9
- routes: int32 [8192, 2], P(('grp', 'ep')), parts along dimension 0, may hold values from 0 to 15, all different within a row; in each aligned block of 256 rows (0 to 255, 256 to 511, ...) at most 40 rows name the same one
- route_weights: float32 [8192, 2], P(('grp', 'ep')), parts along dimension 0, may hold values from 0.2 to 1.5
- expert_gate: bfloat16 [16, 2048, 256], P('ep'), may hold values from -0.125 to 0.125
- expert_up: bfloat16 [16, 2048, 256], P('ep'), may hold values from -0.125 to 0.125
- expert_down: bfloat16 [16, 256, 2048], P('ep'), may hold values from -0.375 to 0.375
- shared_gate: bfloat16 [2048, 256], replicated, may hold values from -0.125 to 0.125
- shared_up: bfloat16 [2048, 256], replicated, may hold values from -0.125 to 0.125
- shared_down: bfloat16 [256, 2048], replicated, may hold values from -0.375 to 0.375
Outputs:
- mixed: bfloat16 [8192, 2048], P(('grp', 'ep')), parts along dimension 0
The draws below stay inside these ranges and needn't reach their ends.
There are 2 independent parts, one for each index of `grp`. The reference program is written for one: setup_inputs(seed, part) draws one part's arguments, and reference() takes and returns one part's arrays. A program takes and returns all parts, laid end to end along the dimension named above; an argument that names none is the same for every part. Nothing has to cross between parts.
Inputs may be any that keep to these rules, and one draw needn't show every extreme that they name: `routes`: the 2 experts of a token are distinct. Among the tokens of one device, at most 40 choose any one expert; in every draw some expert is chosen by exactly 40 tokens of some device.
All inputs are finite; a program needn't handle non-finite values.
Results may differ from the reference program's by a relative error of at most 0.0075.
Values may be sent and summed in bfloat16 or wider, within the bound.
A program may use at most 64 MiB of HBM per device.

```python
import math
import jax
import jax.numpy as jnp
import numpy as np
from jax import lax

D = 2048
DE = 256
DS = 256
TOP_K = 2
TOK_DEV = 256
EXPERTS = 16
TOKENS = 4096
CAPACITY = 40
N_EP = 16


def block_levels(key, dims, cuts, least, largest):
    loudness, own = 1.0, jax.random.fold_in(key, 6)
    for dim, parts in cuts:
        draws = jnp.exp(jax.random.uniform(jax.random.fold_in(own, dim), (parts,), jnp.float32, least / len(cuts), largest / len(cuts)))
        loudness = loudness * jnp.repeat(draws, dims[dim] // parts).reshape([-1 if axis == dim else 1 for axis in range(len(dims))])
    return loudness


def routed_block(key, own, number, rows, amount, top, most, skew):
    sequence = jax.random.permutation(key, amount)
    heavy_load, common = load_shares(amount, rows * top, most, skew, True), load_shares(amount, rows * top, most, skew, False)
    places = jnp.arange(amount)

    def named(tallies, rotation):
        used = int((tallies > 0).sum())
        fixed = max(1, used // 4)
        passed = fixed + (places - fixed + rotation * (used - fixed)) % max(1, amount - fixed)
        return jnp.zeros((amount,), jnp.int32).at[sequence[jnp.where(places < fixed, places, passed)]].set(jnp.asarray(tallies, jnp.int32))

    tallies = jnp.where(number % 4 == 0, named(heavy_load, number // 4), named(common, number - number // 4 - 1))
    mixed = jax.random.permutation(jax.random.fold_in(own, 3), amount)
    source_of, taker = mixed[0:amount // 2 * 2:2], mixed[1:amount // 2 * 2:2]
    room = jnp.minimum(tallies[source_of] - 1, most - tallies[taker]) // 2
    room = jnp.where((source_of == sequence[0]) | (taker == sequence[0]) | (tallies[taker] == 0), 0, jnp.maximum(room, 0))
    passed = jax.random.randint(jax.random.fold_in(own, 4), (amount // 2,), 0, 1 << 20) % (room + 1)
    tallies = tallies.at[source_of].add(-passed).at[taker].add(passed)
    labels = jnp.searchsorted(jnp.cumsum(tallies), jnp.arange(rows * top), side="right").astype(jnp.int32)
    table = labels.reshape(top, rows).T
    table = table[jax.random.permutation(jax.random.fold_in(own, 1), rows)]
    rotation = jax.random.randint(jax.random.fold_in(own, 2), (rows, 1), 0, top)
    return jnp.take_along_axis(table, (jnp.arange(top)[None, :] + rotation) % top, axis=1)


def load_shares(number_of, total, reach, skew, full):
    weights = [(1 << 20) // math.isqrt(grade ** skew) + 1 for grade in range(1, number_of + 1)]
    largest = reach if full else min(reach, max(-(-total // number_of), total * weights[0] // sum(weights)))
    least = 1 if total - largest >= number_of - 1 else 0
    holding, rest = [largest] + [least] * (number_of - 1), total - largest - least * (number_of - 1)
    while rest > 0:
        movable = [i for i in range(1, number_of) if holding[i] < largest] or [i for i in range(1, number_of) if holding[i] < reach]
        whole, left = sum([weights[i] for i in movable]), rest
        for i in movable:
            addition = min(reach - holding[i], max(1, left * weights[i] // whole), rest)
            holding[i] = holding[i] + addition
            rest = rest - addition
    return np.array(holding)


def centred(own_key, dims, spread, limit, shards=(), kind=jnp.bfloat16):
    values = spread * jax.random.normal(own_key, dims, jnp.float32)
    if shards:
        values = values * block_levels(own_key, dims, shards, -0.22, 0.18)
    return jnp.clip(values, -limit, limit).astype(kind)


def setup_inputs(seed: int = 0, part: int = 0) -> dict:
    key_of = jax.random.split(jax.random.key(seed), 11)
    own_keys = jax.random.split(jax.random.fold_in(key_of[10], part), 11)
    tokens = centred(own_keys[0], (TOKENS, D), 1.0, 6.0, ((0, 16),))
    norm_gain = jnp.clip(1.0 + 0.18 * jax.random.normal(key_of[1], (D,), jnp.float32), 0.1, 1.9)
    routes_keys = jax.random.split(jax.random.fold_in(own_keys[2], 1), TOKENS // TOK_DEV)
    routes_turns = jax.random.permutation(jax.random.fold_in(own_keys[2], 3), TOKENS // TOK_DEV)
    routes = jax.vmap(lambda own, number: routed_block(jax.random.fold_in(own_keys[2], 2), own, number, TOK_DEV, EXPERTS, TOP_K, CAPACITY, 2))(routes_keys, routes_turns).reshape((TOKENS, TOP_K))
    route_weights = jnp.clip(0.2 + 1.3 * jax.random.uniform(own_keys[3], (TOKENS, TOP_K), jnp.float32) ** block_levels(own_keys[3], (TOKENS, TOP_K), ((0, 16),), -0.2, 0.2), 0.2, 1.5)
    expert_gate = centred(key_of[4], (EXPERTS, D, DE), D ** -0.5, 0.125, ((0, 16),))
    expert_up = centred(key_of[5], (EXPERTS, D, DE), D ** -0.5, 0.125, ((0, 16),))
    expert_down = centred(key_of[6], (EXPERTS, DE, D), DE ** -0.5, 0.375, ((0, 16),))
    shared_gate = centred(key_of[7], (D, DS), D ** -0.5, 0.125)
    shared_up = centred(key_of[8], (D, DS), D ** -0.5, 0.125)
    shared_down = centred(key_of[9], (DS, D), DS ** -0.5, 0.375)
    return dict(tokens=tokens, norm_gain=norm_gain, routes=routes, route_weights=route_weights, expert_gate=expert_gate, expert_up=expert_up, expert_down=expert_down, shared_gate=shared_gate, shared_up=shared_up, shared_down=shared_down)


def swiglu_rows(row_block, w_gate, w_up, w_down):
    gate_part = jnp.dot(row_block, w_gate, preferred_element_type=jnp.float32)
    up_part = jnp.dot(row_block, w_up, preferred_element_type=jnp.float32)
    hidden = (jax.nn.silu(gate_part) * up_part).astype(jnp.bfloat16)
    return jnp.dot(hidden, w_down, preferred_element_type=jnp.float32)

def reference(tokens, norm_gain, routes, route_weights, expert_gate, expert_up, expert_down, shared_gate, shared_up, shared_down):
    upcast = tokens.astype(jnp.float32)
    factor = lax.rsqrt(lax.optimization_barrier(jnp.mean(upcast * upcast, axis=-1, keepdims=True)) + 1e-06)
    normed = (upcast * factor * norm_gain.astype(jnp.float32)).astype(jnp.bfloat16)
    pair_count = TOKENS * TOP_K
    flat_expert = routes.reshape(-1).astype(jnp.int32)
    onehot = (flat_expert[:, None] == jnp.arange(EXPERTS, dtype=jnp.int32)[None, :]).astype(jnp.int32)
    position = (lax.optimization_barrier(jnp.sum(jnp.cumsum(onehot, axis=0) * onehot, axis=1)) - 1).astype(jnp.int32)
    per_expert = N_EP * CAPACITY
    slot_index = (flat_expert * per_expert + position).astype(jnp.int32)
    pair_token = (jnp.arange(pair_count, dtype=jnp.int32) // TOP_K).astype(jnp.int32)
    slot_token = jnp.full((EXPERTS * per_expert,), TOKENS, jnp.int32).at[slot_index].set(pair_token)
    padded = jnp.concatenate([normed, jnp.zeros((1, D), jnp.bfloat16)], axis=0)

    def one_expert(args):
        table, w_gate, w_up, w_down = args
        return swiglu_rows(padded[table], w_gate, w_up, w_down).astype(jnp.bfloat16)
    outputs = lax.map(one_expert, (slot_token.reshape(EXPERTS, per_expert), expert_gate, expert_up, expert_down))
    pair_out = outputs.reshape(EXPERTS * per_expert, D)[slot_index].astype(jnp.float32).reshape(TOKENS, TOP_K, D)
    routed = lax.optimization_barrier(jnp.sum(pair_out * route_weights[:, :, None], axis=1))
    shared = swiglu_rows(normed, shared_gate, shared_up, shared_down)
    return (routed + shared).astype(jnp.bfloat16)
```

```python
import functools

import jax
import jax.numpy as jnp
from jax import lax
from jax.experimental import pallas as pl
from jax.experimental.pallas import tpu as pltpu
from jax.sharding import PartitionSpec as P

BF16 = jnp.bfloat16
F32 = jnp.float32
PIECES = 2


def dot(a, b, dims=((1,), (0,))):
    return lax.dot_general(a, b, (dims, ((), ())), preferred_element_type=F32)


def hidden_rows(rows, w_gate, w_up):
    gate_part = dot(rows, w_gate)
    up_part = dot(rows, w_up)
    return (gate_part / (1.0 + jnp.exp(-gate_part)) * up_part).astype(BF16)


def kernel(
    n, groups, cap,
    tokens_hbm, gain_ref, routes_ref, rw_ref, eg_hbm, eu_hbm, ed_hbm, sg_hbm, su_hbm, sd_hbm,
    out_ref,
    tok, normed, place, scale, wg, wu, wd, fg, fu, fd, sg, su, sd, obuf, arr, ybuf, ret, acc,
    load_sem, wsend, wrecv, xsend, xrecv, dsend, drecv, rsend, rrecv,
):
    half = n // 2
    me = lax.axis_index("ep")
    grp = lax.axis_index("grp")
    base = (me // half) * half
    mine = me % half
    far = (me + half) % n
    rows = tok.shape[0]
    width = tok.shape[1]

    def peer(j):
        total, bit = 0, 1
        while bit < half:
            total = total + bit * (((mine // bit) % 2 + (j // bit) % 2) % 2)
            bit *= 2
        return total

    barrier = pltpu.get_barrier_semaphore()

    def greet(i, c):
        pl.semaphore_signal(barrier, inc=1, device_id={"ep": base + peer(i)})
        return c

    lax.fori_loop(1, half, greet, 0)
    pl.semaphore_signal(barrier, inc=1, device_id={"ep": far})
    for k in range(1, groups):
        pl.semaphore_signal(barrier, inc=1, device_id={"grp": (grp + k) % groups})

    loads = [(tokens_hbm, tok), (eg_hbm.at[0], wg), (eu_hbm.at[0], wu), (ed_hbm.at[0], wd),
             (sg_hbm, sg), (su_hbm, su), (sd_hbm, sd)]
    loads = [pltpu.make_async_copy(a, b, load_sem.at[i]) for i, (a, b) in enumerate(loads)]
    for copy in loads:
        copy.start()

    def share(group, array, piece):
        depth = array.shape[-2] // groups // PIECES
        start = (group * PIECES + piece) * depth
        return pl.ds(pl.multiple_of(start, depth), depth)

    def weight_copy(a, piece):
        src, dst = ((eg_hbm, fg), (eu_hbm, fu), (ed_hbm, fd))[a]
        where = share(grp, dst, piece)
        return pltpu.make_async_remote_copy(
            src_ref=src.at[0, where], dst_ref=dst.at[where],
            send_sem=wsend.at[a * PIECES + piece], recv_sem=wrecv.at[a * PIECES + piece],
            device_id={"ep": far})

    def forward_copy(a, piece, k):
        dst = (fg, fu, fd)[a]
        where = share(grp, dst, piece)
        i = (a * PIECES + piece) * max(1, groups - 1) + k - 1
        return pltpu.make_async_remote_copy(
            src_ref=dst.at[where], dst_ref=dst.at[where],
            send_sem=xsend.at[i], recv_sem=xrecv.at[i],
            device_id={"grp": (grp + k) % groups})

    pl.semaphore_wait(barrier, half - 1 + 1 + groups - 1)
    chunks = [(a, piece) for a in range(3) for piece in range(PIECES)]
    for a, piece in chunks:
        weight_copy(a, piece).start()

    lane = lax.broadcasted_iota(jnp.int32, (rows, 128), 1)
    chosen = jnp.zeros((rows, 128), F32)
    weight = jnp.zeros((rows, 128), F32)
    for k in range(routes_ref.shape[1]):
        hit = lane == routes_ref[:, k:k + 1]
        chosen = chosen + jnp.where(hit, 1.0, 0.0)
        weight = weight + jnp.where(hit, rw_ref[:, k:k + 1], 0.0)
    chosen_t = chosen.T
    earlier = (lax.broadcasted_iota(jnp.int32, (rows, rows), 0)
               < lax.broadcasted_iota(jnp.int32, (rows, rows), 1))
    before = dot(chosen_t.astype(BF16), jnp.where(earlier, 1.0, 0.0).astype(BF16))
    place[...] = jnp.where(chosen_t > 0.5, before, -1.0)
    scale[...] = weight.T

    loads[0].wait()

    def norm_step(i, c):
        at = pl.ds(pl.multiple_of(i * 32, 32), 32)
        x = tok[at, :].astype(F32)
        factor = lax.rsqrt(jnp.mean(x * x, axis=-1, keepdims=True) + 1e-06)
        normed[at, :] = (x * factor * gain_ref[...]).astype(BF16)
        return c

    lax.fori_loop(0, rows // 32, norm_step, 0)
    slot = lax.broadcasted_iota(jnp.int32, (cap, rows), 0).astype(F32)

    def gather(p):
        ours = slot == place[pl.ds(base + p, 1), :]
        theirs = slot == place[pl.ds((base + half) % n + p, 1), :]
        pick = jnp.concatenate([jnp.where(ours, 1.0, 0.0), jnp.where(theirs, 1.0, 0.0)], axis=0)
        got = dot(pick.astype(BF16), normed[...])
        return got[:cap].astype(BF16), got[cap:].astype(BF16)

    def dispatch_copy(p):
        return pltpu.make_async_remote_copy(
            src_ref=obuf.at[p], dst_ref=arr.at[mine],
            send_sem=dsend.at[p], recv_sem=drecv.at[mine], device_id={"ep": base + p})

    def dispatch_wait(p):
        pltpu.make_async_remote_copy(
            src_ref=obuf.at[p], dst_ref=arr.at[p],
            send_sem=dsend.at[p], recv_sem=drecv.at[p], device_id={"ep": base + p}).wait_recv()

    def return_copy(p, b):
        return pltpu.make_async_remote_copy(
            src_ref=ybuf.at[p, b], dst_ref=ret.at[mine, b],
            send_sem=rsend.at[p, b], recv_sem=rrecv.at[mine, b], device_id={"ep": base + p})

    def return_wait(p, b):
        pltpu.make_async_remote_copy(
            src_ref=ybuf.at[p, b], dst_ref=ret.at[p, b],
            send_sem=rsend.at[p, b], recv_sem=rrecv.at[p, b], device_id={"ep": base + p}).wait_recv()

    def dispatch_step(i, c):
        p = peer(half - 1 - i)
        first, second = gather(p)
        obuf[p, 0] = first
        obuf[p, 1] = second
        dispatch_copy(p).start()
        return c

    lax.fori_loop(0, half - 1, dispatch_step, 0)
    first, second = gather(mine)
    arr[mine, 0] = first
    arr[mine, 1] = second

    for copy in loads[4:]:
        copy.wait()
    acc[...] = dot(hidden_rows(normed[...], sg[...], su[...]), sd[...])
    for copy in loads[1:4]:
        copy.wait()

    def combine(p, b):
        e = (base + b * half) % n + p
        pick = jnp.where(slot == place[pl.ds(e, 1), :], scale[pl.ds(e, 1), :], 0.0)
        acc[...] += dot(pick.astype(BF16), ret[p, b], ((0,), (0,)))

    def own_step(i, c):
        p = peer(half - 1 - i)
        dispatch_wait(p)
        ybuf[p, 0] = dot(hidden_rows(arr[p, 0], wg[...], wu[...]), wd[...]).astype(BF16)
        return_copy(p, 0).start()
        return c

    def forward(a, piece):
        weight_copy(a, piece).wait_recv()
        for k in range(1, groups):
            forward_copy(a, piece, k).start()

    done = 0
    for i, (a, piece) in enumerate(chunks):
        until = (half - 1) * (i + 1) // len(chunks)
        lax.fori_loop(done, until, own_step, 0)
        done = until
        forward(a, piece)
    ret[mine, 0] = dot(hidden_rows(arr[mine, 0], wg[...], wu[...]), wd[...]).astype(BF16)

    for a, piece in chunks:
        for k in range(1, groups):
            forward_copy(a, piece, k).wait_recv()

    def far_step(i, c):
        p = peer(half - 1 - i)
        ybuf[p, 1] = dot(hidden_rows(arr[p, 1], fg[...], fu[...]), fd[...]).astype(BF16)
        return_copy(p, 1).start()
        return c

    lax.fori_loop(0, half - 1, far_step, 0)
    ret[mine, 1] = dot(hidden_rows(arr[mine, 1], fg[...], fu[...]), fd[...]).astype(BF16)

    combine(mine, 0)
    combine(mine, 1)
    for b in range(2):

        def combine_step(i, c):
            p = peer(half - 1 - i)
            return_wait(p, b)
            combine(p, b)
            return c

        lax.fori_loop(0, half - 1, combine_step, 0)
    out_ref[...] = acc[...].astype(BF16)

    def drain(i, c):
        p = peer(half - 1 - i)
        dispatch_copy(p).wait_send()
        return_copy(p, 0).wait_send()
        return_copy(p, 1).wait_send()
        return c

    lax.fori_loop(0, half - 1, drain, 0)
    for a, piece in chunks:
        weight_copy(a, piece).wait_send()
        for k in range(1, groups):
            forward_copy(a, piece, k).wait_send()


def on_device(tokens, norm_gain, routes, route_weights, expert_gate, expert_up, expert_down,
              shared_gate, shared_up, shared_down):
    rows, width = tokens.shape
    n, groups = lax.axis_size("ep"), lax.axis_size("grp")
    half = n // 2
    cap = -(-(5 * rows * routes.shape[1] // (4 * n)) // 8) * 8
    nchunk = 3 * PIECES
    nfwd = nchunk * max(1, groups - 1)
    vmem = lambda shape, kind=BF16: pltpu.VMEM(shape, kind)
    anyspec = pl.BlockSpec(memory_space=pl.ANY)
    vspec = pl.BlockSpec(memory_space=pltpu.VMEM)
    block = (half, 2, cap, width)
    return pl.pallas_call(
        functools.partial(kernel, n, groups, cap),
        out_shape=jax.ShapeDtypeStruct((rows, width), BF16),
        in_specs=[anyspec, vspec, vspec, vspec] + [anyspec] * 6,
        out_specs=vspec,
        scratch_shapes=[
            vmem((rows, width)), vmem((rows, width)), vmem((128, rows), F32), vmem((128, rows), F32),
            vmem(expert_gate.shape[1:]), vmem(expert_up.shape[1:]), vmem(expert_down.shape[1:]),
            vmem(expert_gate.shape[1:]), vmem(expert_up.shape[1:]), vmem(expert_down.shape[1:]),
            vmem(shared_gate.shape), vmem(shared_up.shape), vmem(shared_down.shape),
            vmem(block), vmem(block), vmem(block), vmem(block), vmem((rows, width), F32),
            pltpu.SemaphoreType.DMA((7,)),
            pltpu.SemaphoreType.DMA((nchunk,)), pltpu.SemaphoreType.DMA((nchunk,)),
            pltpu.SemaphoreType.DMA((nfwd,)), pltpu.SemaphoreType.DMA((nfwd,)),
            pltpu.SemaphoreType.DMA((half,)), pltpu.SemaphoreType.DMA((half,)),
            pltpu.SemaphoreType.DMA((half, 2)), pltpu.SemaphoreType.DMA((half, 2)),
        ],
        compiler_params=pltpu.CompilerParams(
            collective_id=0, has_side_effects=True, vmem_limit_bytes=60 * 1024 * 1024),
    )(tokens, norm_gain.reshape(1, width), routes, route_weights, expert_gate, expert_up,
      expert_down, shared_gate, shared_up, shared_down)


def solution(mesh):
    return jax.shard_map(
        on_device,
        mesh=mesh,
        in_specs=(
            P(("grp", "ep"), None),
            P(),
            P(("grp", "ep"), None),
            P(("grp", "ep"), None),
            P("ep", None, None),
            P("ep", None, None),
            P("ep", None, None),
            P(),
            P(),
            P(),
        ),
        out_specs=P(("grp", "ep"), None),
        check_vma=False,
    )
```

```python
import functools

import jax
import jax.numpy as jnp
from jax import lax
from jax.experimental import pallas as pl
from jax.experimental.pallas import tpu as pltpu
from jax.sharding import PartitionSpec as P

BF16 = jnp.bfloat16
F32 = jnp.float32
PIECES = 2
SLABS = 4


def dot(a, b, dims=((1,), (0,))):
    return lax.dot_general(a, b, (dims, ((), ())), preferred_element_type=F32)


def hidden_rows(rows, w_gate, w_up):
    gate_part = dot(rows, w_gate)
    up_part = dot(rows, w_up)
    return (gate_part / (1.0 + jnp.exp(-gate_part)) * up_part).astype(BF16)


def kernel(
    n, groups, cap,
    tokens_hbm, gain_ref, routes_ref, rw_ref, eg_hbm, eu_hbm, ed_hbm, sg_hbm, su_hbm, sd_hbm,
    out_ref,
    tok, normed, place, scale, wg, wu, wd, fg, fu, fd, sg, su, sd, obuf, arr, ybuf, ret, acc, hid, pick,
    load_sem, wsend, wrecv, xsend, xrecv, dsend, drecv, rsend, rrecv,
):
    half = n // 2
    me = lax.axis_index("ep")
    grp = lax.axis_index("grp")
    base = (me // half) * half
    mine = me % half
    far = (me + half) % n
    rows = tok.shape[0]
    width = tok.shape[1]

    def peer(j):
        total, bit = 0, 1
        while bit < half:
            total = total + bit * (((mine // bit) % 2 + (j // bit) % 2) % 2)
            bit *= 2
        return total

    capp = ret.shape[2]
    if capp > cap:
        low = cap // 16 * 16
        ret[:, :, low:, :] = jnp.zeros((2, half, capp - low, width), BF16)
    barrier = pltpu.get_barrier_semaphore()

    def greet(i, c):
        pl.semaphore_signal(barrier, inc=1, device_id={"ep": base + peer(i)})
        return c

    lax.fori_loop(1, half, greet, 0)
    pl.semaphore_signal(barrier, inc=1, device_id={"ep": far})
    for k in range(1, groups):
        pl.semaphore_signal(barrier, inc=1, device_id={"grp": (grp + k) % groups})

    loads = [(tokens_hbm, tok), (eg_hbm.at[0], wg), (eu_hbm.at[0], wu), (ed_hbm.at[0], wd),
             (sg_hbm, sg), (su_hbm, su), (sd_hbm, sd)]
    loads = [pltpu.make_async_copy(a, b, load_sem.at[i]) for i, (a, b) in enumerate(loads)]
    for copy in loads:
        copy.start()

    slab = width // SLABS

    def region(group, a, piece):
        depth = (fg, fu, fd)[a].shape[0] // groups
        if a == 2:
            return pl.ds(pl.multiple_of(group * depth, depth), depth), pl.ds(piece * slab, slab)
        depth = depth // PIECES
        start = (group * PIECES + piece) * depth
        return pl.ds(pl.multiple_of(start, depth), depth), pl.ds(0, fg.shape[1])

    chunks = [(a, piece) for piece in range(PIECES) for a in range(2)]
    chunks += [(2, piece) for piece in range(SLABS)]

    def weight_copy(a, piece):
        src, dst = ((eg_hbm, fg), (eu_hbm, fu), (ed_hbm, fd))[a]
        at, i = region(grp, a, piece), chunks.index((a, piece))
        return pltpu.make_async_remote_copy(
            src_ref=src.at[0, at[0], at[1]], dst_ref=dst.at[at[0], at[1]],
            send_sem=wsend.at[i], recv_sem=wrecv.at[i], device_id={"ep": far})

    def forward_copy(a, piece, k):
        dst = (fg, fu, fd)[a]
        at = region(grp, a, piece)
        i = chunks.index((a, piece)) * max(1, groups - 1) + k - 1
        return pltpu.make_async_remote_copy(
            src_ref=dst.at[at[0], at[1]], dst_ref=dst.at[at[0], at[1]],
            send_sem=xsend.at[i], recv_sem=xrecv.at[i],
            device_id={"grp": (grp + k) % groups})

    pl.semaphore_wait(barrier, half - 1 + 1 + groups - 1)
    weight_copy(*chunks[0]).start()

    lane = lax.broadcasted_iota(jnp.int32, (rows, 128), 1)
    chosen = jnp.zeros((rows, 128), F32)
    weight = jnp.zeros((rows, 128), F32)
    for k in range(routes_ref.shape[1]):
        hit = lane == routes_ref[:, k:k + 1]
        chosen = chosen + jnp.where(hit, 1.0, 0.0)
        weight = weight + jnp.where(hit, rw_ref[:, k:k + 1], 0.0)
    chosen_t = chosen.T
    earlier = (lax.broadcasted_iota(jnp.int32, (rows, rows), 0)
               < lax.broadcasted_iota(jnp.int32, (rows, rows), 1))
    before = dot(chosen_t.astype(BF16), jnp.where(earlier, 1.0, 0.0).astype(BF16))
    place[...] = jnp.where(chosen_t > 0.5, before, -1.0)
    scale[...] = weight.T

    loads[0].wait()

    def norm_step(i, c):
        at = pl.ds(pl.multiple_of(i * 32, 32), 32)
        x = tok[at, :].astype(F32)
        factor = lax.rsqrt(jnp.mean(x * x, axis=-1, keepdims=True) + 1e-06)
        normed[at, :] = (x * factor * gain_ref[...]).astype(BF16)
        return c

    lax.fori_loop(0, rows // 32, norm_step, 0)
    slot = lax.broadcasted_iota(jnp.int32, (capp, rows), 0).astype(F32)
    slot = jnp.where(slot < cap, slot, -2.0)

    def gather(p):
        ours = slot == place[pl.ds(base + p, 1), :]
        theirs = slot == place[pl.ds((base + half) % n + p, 1), :]
        want = jnp.concatenate([jnp.where(ours, 1.0, 0.0), jnp.where(theirs, 1.0, 0.0)], axis=0)
        got = dot(want.astype(BF16), normed[...])
        return got[:capp].astype(BF16), got[capp:].astype(BF16)

    used = pl.ds(0, cap)

    def dispatch_copy(p):
        return pltpu.make_async_remote_copy(
            src_ref=obuf.at[:, p, used], dst_ref=arr.at[:, mine, used],
            send_sem=dsend.at[p], recv_sem=drecv.at[mine], device_id={"ep": base + p})

    def dispatch_wait(p):
        pltpu.make_async_remote_copy(
            src_ref=obuf.at[:, p, used], dst_ref=arr.at[:, p, used],
            send_sem=dsend.at[p], recv_sem=drecv.at[p], device_id={"ep": base + p}).wait_recv()

    def message(ref, p, m):
        if m == 0:
            return ref.at[0, p, used]
        return ref.at[1, p, used, pl.ds((m - 1) * slab, slab)]

    def return_copy(p, m):
        return pltpu.make_async_remote_copy(
            src_ref=message(ybuf, p, m), dst_ref=message(ret, mine, m),
            send_sem=rsend.at[p, m], recv_sem=rrecv.at[mine, m], device_id={"ep": base + p})

    def return_wait(p, m):
        pltpu.make_async_remote_copy(
            src_ref=message(ybuf, p, m), dst_ref=message(ret, p, m),
            send_sem=rsend.at[p, m], recv_sem=rrecv.at[p, m],
            device_id={"ep": base + p}).wait_recv()

    def dispatch_step(i, c):
        p = peer(half - 1 - i)
        first, second = gather(p)
        obuf[0, p] = first
        obuf[1, p] = second
        dispatch_copy(p).start()
        return c

    lax.fori_loop(0, half - 1, dispatch_step, 0)
    for a, piece in chunks[1:]:
        weight_copy(a, piece).start()
    first, second = gather(mine)
    arr[0, mine] = first
    arr[1, mine] = second

    for copy in loads[4:]:
        copy.wait()
    acc[...] = dot(hidden_rows(normed[...], sg[...], su[...]), sd[...])
    for copy in loads[1:4]:
        copy.wait()

    for b in range(2):
        for p in range(half):
            at = pl.ds((base + b * half) % n + p, 1)
            want = jnp.where(slot == place[at, :], scale[at, :], 0.0)
            pick[b, p * capp:(p + 1) * capp, :] = want.astype(BF16)

    def own_step(i, c):
        p = peer(i + 1)
        dispatch_wait(p)
        ybuf[0, p] = dot(hidden_rows(arr[0, p], wg[...], wu[...]), wd[...]).astype(BF16)
        return_copy(p, 0).start()
        return c

    def forward(a, piece):
        weight_copy(a, piece).wait_recv()
        for k in range(1, groups):
            forward_copy(a, piece, k).start()

    def forwarded(a, piece):
        for k in range(1, groups):
            forward_copy(a, piece, k).wait_recv()

    early = chunks[:-SLABS]
    done = 0
    for i, (a, piece) in enumerate(early):
        until = (half - 1) * (i + 1) // len(early)
        lax.fori_loop(done, until, own_step, 0)
        done = until
        forward(a, piece)
    own = dot(hidden_rows(arr[0, mine], wg[...], wu[...]), wd[...]).astype(BF16)
    ret[0, mine] = own

    for a, piece in early:
        forwarded(a, piece)
    hid[...] = hidden_rows(arr[1].reshape(half * capp, width), fg[...], fu[...])

    def far_slab(c):
        forwarded(2, c)
        cols = pl.ds(c * slab, slab)
        got = dot(hid[...], fd[:, cols]).astype(BF16)
        ybuf[1, :, :, cols] = got.reshape(half, capp, slab)

        def send(i, k):
            return_copy(peer(half - 1 - i), 1 + c).start()
            return k

        lax.fori_loop(0, half - 1, send, 0)
        local = pl.ds(pl.multiple_of(mine * capp, capp), capp)
        ret[1, mine, :, cols] = dot(hid[local, :], fd[:, cols]).astype(BF16)

    for c in range(SLABS):
        forward(2, c)
        if c > 0:
            far_slab(c - 1)
    far_slab(SLABS - 1)

    def arrive(m):
        def step(i, k):
            return_wait(peer(i + 1), m)
            return k

        lax.fori_loop(0, half - 1, step, 0)

    arrive(0)
    acc[...] += dot(pick[0], ret[0].reshape(half * capp, width), ((0,), (0,)))
    for c in range(SLABS):
        arrive(1 + c)
        cols = pl.ds(c * slab, slab)
        total = acc[:, cols] + dot(
            pick[1], ret[1, :, :, cols].reshape(half * capp, slab), ((0,), (0,)))
        out_ref[:, cols] = total.astype(BF16)

    def drain(i, c):
        p = peer(half - 1 - i)
        dispatch_copy(p).wait_send()
        for m in range(1 + SLABS):
            return_copy(p, m).wait_send()
        return c

    lax.fori_loop(0, half - 1, drain, 0)
    for a, piece in chunks:
        weight_copy(a, piece).wait_send()
        for k in range(1, groups):
            forward_copy(a, piece, k).wait_send()


def on_device(tokens, norm_gain, routes, route_weights, expert_gate, expert_up, expert_down,
              shared_gate, shared_up, shared_down):
    rows, width = tokens.shape
    n, groups = lax.axis_size("ep"), lax.axis_size("grp")
    half = n // 2
    cap = -(-(5 * rows * routes.shape[1] // (4 * n)) // 8) * 8
    nchunk = 2 * PIECES + SLABS
    nfwd = nchunk * max(1, groups - 1)
    vmem = lambda shape, kind=BF16: pltpu.VMEM(shape, kind)
    anyspec = pl.BlockSpec(memory_space=pl.ANY)
    vspec = pl.BlockSpec(memory_space=pltpu.VMEM)
    capp = -(-cap // 16) * 16
    block = (2, half, capp, width)
    return pl.pallas_call(
        functools.partial(kernel, n, groups, cap),
        out_shape=jax.ShapeDtypeStruct((rows, width), BF16),
        in_specs=[anyspec, vspec, vspec, vspec] + [anyspec] * 6,
        out_specs=vspec,
        scratch_shapes=[
            vmem((rows, width)), vmem((rows, width)), vmem((128, rows), F32), vmem((128, rows), F32),
            vmem(expert_gate.shape[1:]), vmem(expert_up.shape[1:]), vmem(expert_down.shape[1:]),
            vmem(expert_gate.shape[1:]), vmem(expert_up.shape[1:]), vmem(expert_down.shape[1:]),
            vmem(shared_gate.shape), vmem(shared_up.shape), vmem(shared_down.shape),
            vmem(block), vmem(block), vmem(block), vmem(block), vmem((rows, width), F32),
            vmem((half * capp, expert_gate.shape[2])), vmem((2, half * capp, rows)),
            pltpu.SemaphoreType.DMA((7,)),
            pltpu.SemaphoreType.DMA((nchunk,)), pltpu.SemaphoreType.DMA((nchunk,)),
            pltpu.SemaphoreType.DMA((nfwd,)), pltpu.SemaphoreType.DMA((nfwd,)),
            pltpu.SemaphoreType.DMA((half,)), pltpu.SemaphoreType.DMA((half,)),
            pltpu.SemaphoreType.DMA((half, 1 + SLABS)), pltpu.SemaphoreType.DMA((half, 1 + SLABS)),
        ],
        compiler_params=pltpu.CompilerParams(
            collective_id=0, has_side_effects=True, vmem_limit_bytes=60 * 1024 * 1024),
    )(tokens, norm_gain.reshape(1, width), routes, route_weights, expert_gate, expert_up,
      expert_down, shared_gate, shared_up, shared_down)


def solution(mesh):
    return jax.shard_map(
        on_device,
        mesh=mesh,
        in_specs=(
            P(("grp", "ep"), None),
            P(),
            P(("grp", "ep"), None),
            P(("grp", "ep"), None),
            P("ep", None, None),
            P("ep", None, None),
            P("ep", None, None),
            P(),
            P(),
            P(),
        ),
        out_specs=P(("grp", "ep"), None),
        check_vma=False,
    )
```

```python
import functools

import jax
import jax.numpy as jnp
from jax import lax
from jax.experimental import pallas as pl
from jax.experimental.pallas import tpu as pltpu
from jax.sharding import PartitionSpec as P

BF16 = jnp.bfloat16
F32 = jnp.float32
PIECES = 2
SLABS = 4


def dot(a, b, dims=((1,), (0,))):
    return lax.dot_general(a, b, (dims, ((), ())), preferred_element_type=F32)


def hidden_rows(rows, w_gate, w_up):
    gate_part = dot(rows, w_gate)
    up_part = dot(rows, w_up)
    return (gate_part / (1.0 + jnp.exp(-gate_part)) * up_part).astype(BF16)


def kernel(
    n, groups, cap,
    tokens_hbm, gain_ref, routes_ref, rw_ref, eg_hbm, eu_hbm, ed_hbm, sg_hbm, su_hbm, sd_hbm,
    out_ref,
    tok, normed, place, scale, wg, wu, wd, fg, fu, fd, sg, su, sd, obuf, arr, ybuf, ret, acc, hid, pick,
    load_sem, wsend, wrecv, xsend, xrecv, dsend, drecv, rsend, rrecv,
):
    half = n // 2
    me = lax.axis_index("ep")
    grp = lax.axis_index("grp")
    base = (me // half) * half
    mine = me % half
    far = (base + half) % n + (mine + half // 2) % half
    rows = tok.shape[0]
    width = tok.shape[1]

    def peer(j):
        total, bit = 0, 1
        while bit < half:
            total = total + bit * (((mine // bit) % 2 + (j // bit) % 2) % 2)
            bit *= 2
        return total

    capp = ret.shape[2]
    if capp > cap:
        low = cap // 16 * 16
        ret[:, :, low:, :] = jnp.zeros((2, half, capp - low, width), BF16)
    barrier = pltpu.get_barrier_semaphore()

    def greet(i, c):
        pl.semaphore_signal(barrier, inc=1, device_id={"ep": base + peer(i)})
        return c

    lax.fori_loop(1, half, greet, 0)
    pl.semaphore_signal(barrier, inc=1, device_id={"ep": far})
    for k in range(1, groups):
        pl.semaphore_signal(barrier, inc=1, device_id={"grp": (grp + k) % groups})

    loads = [(tokens_hbm, tok), (eg_hbm.at[0], wg), (eu_hbm.at[0], wu), (ed_hbm.at[0], wd),
             (sg_hbm, sg), (su_hbm, su), (sd_hbm, sd)]
    loads = [pltpu.make_async_copy(a, b, load_sem.at[i]) for i, (a, b) in enumerate(loads)]
    for copy in loads:
        copy.start()

    slab = width // SLABS

    def region(group, a, piece):
        depth = (fg, fu, fd)[a].shape[0] // groups
        if a == 2:
            return pl.ds(pl.multiple_of(group * depth, depth), depth), pl.ds(piece * slab, slab)
        depth = depth // PIECES
        start = (group * PIECES + piece) * depth
        return pl.ds(pl.multiple_of(start, depth), depth), pl.ds(0, fg.shape[1])

    chunks = [(a, piece) for piece in range(PIECES) for a in range(2)]
    chunks += [(2, piece) for piece in range(SLABS)]

    def weight_copy(a, piece):
        src, dst = ((eg_hbm, fg), (eu_hbm, fu), (ed_hbm, fd))[a]
        at, i = region(grp, a, piece), chunks.index((a, piece))
        return pltpu.make_async_remote_copy(
            src_ref=src.at[0, at[0], at[1]], dst_ref=dst.at[at[0], at[1]],
            send_sem=wsend.at[i], recv_sem=wrecv.at[i], device_id={"ep": far})

    def forward_copy(a, piece, k):
        dst = (fg, fu, fd)[a]
        at = region(grp, a, piece)
        i = chunks.index((a, piece)) * max(1, groups - 1) + k - 1
        return pltpu.make_async_remote_copy(
            src_ref=dst.at[at[0], at[1]], dst_ref=dst.at[at[0], at[1]],
            send_sem=xsend.at[i], recv_sem=xrecv.at[i],
            device_id={"grp": (grp + k) % groups})

    pl.semaphore_wait(barrier, half - 1 + 1 + groups - 1)
    weight_copy(*chunks[0]).start()

    lane = lax.broadcasted_iota(jnp.int32, (rows, 128), 1)
    chosen = jnp.zeros((rows, 128), F32)
    weight = jnp.zeros((rows, 128), F32)
    for k in range(routes_ref.shape[1]):
        hit = lane == routes_ref[:, k:k + 1]
        chosen = chosen + jnp.where(hit, 1.0, 0.0)
        weight = weight + jnp.where(hit, rw_ref[:, k:k + 1], 0.0)
    chosen_t = chosen.T
    earlier = (lax.broadcasted_iota(jnp.int32, (rows, rows), 0)
               < lax.broadcasted_iota(jnp.int32, (rows, rows), 1))
    before = dot(chosen_t.astype(BF16), jnp.where(earlier, 1.0, 0.0).astype(BF16))
    place[...] = jnp.where(chosen_t > 0.5, before, -1.0)
    scale[...] = weight.T

    loads[0].wait()

    def norm_step(i, c):
        at = pl.ds(pl.multiple_of(i * 32, 32), 32)
        x = tok[at, :].astype(F32)
        factor = lax.rsqrt(jnp.mean(x * x, axis=-1, keepdims=True) + 1e-06)
        normed[at, :] = (x * factor * gain_ref[...]).astype(BF16)
        return c

    lax.fori_loop(0, rows // 32, norm_step, 0)
    slot = lax.broadcasted_iota(jnp.int32, (capp, rows), 0).astype(F32)
    slot = jnp.where(slot < cap, slot, -2.0)

    def gather(p):
        ours = slot == place[pl.ds(base + p, 1), :]
        theirs = slot == place[pl.ds((base + half) % n + (p + half // 2) % half, 1), :]
        want = jnp.concatenate([jnp.where(ours, 1.0, 0.0), jnp.where(theirs, 1.0, 0.0)], axis=0)
        got = dot(want.astype(BF16), normed[...])
        return got[:capp].astype(BF16), got[capp:].astype(BF16)

    used = pl.ds(0, cap)

    def dispatch_copy(p):
        return pltpu.make_async_remote_copy(
            src_ref=obuf.at[:, p, used], dst_ref=arr.at[:, mine, used],
            send_sem=dsend.at[p], recv_sem=drecv.at[mine], device_id={"ep": base + p})

    def dispatch_wait(p):
        pltpu.make_async_remote_copy(
            src_ref=obuf.at[:, p, used], dst_ref=arr.at[:, p, used],
            send_sem=dsend.at[p], recv_sem=drecv.at[p], device_id={"ep": base + p}).wait_recv()

    def message(ref, p, m):
        if m == 0:
            return ref.at[0, p, used]
        return ref.at[1, p, used, pl.ds((m - 1) * slab, slab)]

    def return_copy(p, m):
        return pltpu.make_async_remote_copy(
            src_ref=message(ybuf, p, m), dst_ref=message(ret, mine, m),
            send_sem=rsend.at[p, m], recv_sem=rrecv.at[mine, m], device_id={"ep": base + p})

    def return_wait(p, m):
        pltpu.make_async_remote_copy(
            src_ref=message(ybuf, p, m), dst_ref=message(ret, p, m),
            send_sem=rsend.at[p, m], recv_sem=rrecv.at[p, m],
            device_id={"ep": base + p}).wait_recv()

    def dispatch_step(i, c):
        p = peer(half - 1 - i)
        first, second = gather(p)
        obuf[0, p] = first
        obuf[1, p] = second
        dispatch_copy(p).start()
        return c

    lax.fori_loop(0, half - 1, dispatch_step, 0)
    for a, piece in chunks[1:-SLABS]:
        weight_copy(a, piece).start()
    first, second = gather(mine)
    arr[0, mine] = first
    arr[1, mine] = second

    for copy in loads[4:]:
        copy.wait()
    acc[...] = dot(hidden_rows(normed[...], sg[...], su[...]), sd[...])
    for copy in loads[1:4]:
        copy.wait()

    for b in range(2):
        for p in range(half):
            at = pl.ds((base + b * half) % n + (p + b * (half // 2)) % half, 1)
            want = jnp.where(slot == place[at, :], scale[at, :], 0.0)
            pick[b, p * capp:(p + 1) * capp, :] = want.astype(BF16)

    def own_step(i, c):
        p = peer(i + 1)
        dispatch_wait(p)
        ybuf[0, p] = dot(hidden_rows(arr[0, p], wg[...], wu[...]), wd[...]).astype(BF16)
        return_copy(p, 0).start()
        return c

    def forward(a, piece):
        weight_copy(a, piece).wait_recv()
        for k in range(1, groups):
            forward_copy(a, piece, k).start()

    def forwarded(a, piece):
        for k in range(1, groups):
            forward_copy(a, piece, k).wait_recv()

    early = chunks[:-SLABS]
    done = 0
    for i, (a, piece) in enumerate(early):
        until = (half - 1) * (i + 1) // len(early)
        lax.fori_loop(done, until, own_step, 0)
        done = until
        forward(a, piece)
        weight_copy(*chunks[len(early) + i]).start()
    own = dot(hidden_rows(arr[0, mine], wg[...], wu[...]), wd[...]).astype(BF16)
    ret[0, mine] = own

    for a, piece in early:
        forwarded(a, piece)
    hid[...] = hidden_rows(arr[1].reshape(half * capp, width), fg[...], fu[...])

    def far_slab(c):
        forwarded(2, c)
        cols = pl.ds(c * slab, slab)
        got = dot(hid[...], fd[:, cols]).astype(BF16)
        ybuf[1, :, :, cols] = got.reshape(half, capp, slab)

        def send(i, k):
            return_copy(peer(half - 1 - i), 1 + c).start()
            return k

        lax.fori_loop(0, half - 1, send, 0)
        ret[1, mine, :, cols] = ybuf[1, mine, :, cols]

    for c in range(SLABS):
        forward(2, c)
        if c > 0:
            far_slab(c - 1)
    far_slab(SLABS - 1)

    def arrive(m):
        def step(i, k):
            return_wait(peer(i + 1), m)
            return k

        lax.fori_loop(0, half - 1, step, 0)

    arrive(0)
    acc[...] += dot(pick[0], ret[0].reshape(half * capp, width), ((0,), (0,)))
    for c in range(SLABS):
        arrive(1 + c)
        cols = pl.ds(c * slab, slab)
        total = acc[:, cols] + dot(
            pick[1], ret[1, :, :, cols].reshape(half * capp, slab), ((0,), (0,)))
        out_ref[:, cols] = total.astype(BF16)

    def drain(i, c):
        p = peer(half - 1 - i)
        dispatch_copy(p).wait_send()
        for m in range(1 + SLABS):
            return_copy(p, m).wait_send()
        return c

    lax.fori_loop(0, half - 1, drain, 0)
    for a, piece in chunks:
        weight_copy(a, piece).wait_send()
        for k in range(1, groups):
            forward_copy(a, piece, k).wait_send()


def on_device(tokens, norm_gain, routes, route_weights, expert_gate, expert_up, expert_down,
              shared_gate, shared_up, shared_down):
    rows, width = tokens.shape
    n, groups = lax.axis_size("ep"), lax.axis_size("grp")
    half = n // 2
    cap = -(-(5 * rows * routes.shape[1] // (4 * n)) // 8) * 8
    nchunk = 2 * PIECES + SLABS
    nfwd = nchunk * max(1, groups - 1)
    vmem = lambda shape, kind=BF16: pltpu.VMEM(shape, kind)
    anyspec = pl.BlockSpec(memory_space=pl.ANY)
    vspec = pl.BlockSpec(memory_space=pltpu.VMEM)
    capp = cap
    block = (2, half, capp, width)
    return pl.pallas_call(
        functools.partial(kernel, n, groups, cap),
        out_shape=jax.ShapeDtypeStruct((rows, width), BF16),
        in_specs=[anyspec, vspec, vspec, vspec] + [anyspec] * 6,
        out_specs=vspec,
        scratch_shapes=[
            vmem((rows, width)), vmem((rows, width)), vmem((128, rows), F32), vmem((128, rows), F32),
            vmem(expert_gate.shape[1:]), vmem(expert_up.shape[1:]), vmem(expert_down.shape[1:]),
            vmem(expert_gate.shape[1:]), vmem(expert_up.shape[1:]), vmem(expert_down.shape[1:]),
            vmem(shared_gate.shape), vmem(shared_up.shape), vmem(shared_down.shape),
            vmem(block), vmem(block), vmem(block), vmem(block), vmem((rows, width), F32),
            vmem((half * capp, expert_gate.shape[2])), vmem((2, half * capp, rows)),
            pltpu.SemaphoreType.DMA((7,)),
            pltpu.SemaphoreType.DMA((nchunk,)), pltpu.SemaphoreType.DMA((nchunk,)),
            pltpu.SemaphoreType.DMA((nfwd,)), pltpu.SemaphoreType.DMA((nfwd,)),
            pltpu.SemaphoreType.DMA((half,)), pltpu.SemaphoreType.DMA((half,)),
            pltpu.SemaphoreType.DMA((half, 1 + SLABS)), pltpu.SemaphoreType.DMA((half, 1 + SLABS)),
        ],
        compiler_params=pltpu.CompilerParams(
            collective_id=0, has_side_effects=True, vmem_limit_bytes=60 * 1024 * 1024),
    )(tokens, norm_gain.reshape(1, width), routes, route_weights, expert_gate, expert_up,
      expert_down, shared_gate, shared_up, shared_down)


def solution(mesh):
    return jax.shard_map(
        on_device,
        mesh=mesh,
        in_specs=(
            P(("grp", "ep"), None),
            P(),
            P(("grp", "ep"), None),
            P(("grp", "ep"), None),
            P("ep", None, None),
            P("ep", None, None),
            P("ep", None, None),
            P(),
            P(),
            P(),
        ),
        out_specs=P(("grp", "ep"), None),
        check_vma=False,
    )
```

```python
import functools

import jax
import jax.numpy as jnp
from jax import lax
from jax.experimental import pallas as pl
from jax.experimental.pallas import tpu as pltpu
from jax.sharding import PartitionSpec as P

BF16 = jnp.bfloat16
F32 = jnp.float32
PIECES = 2
SLABS = 4


def dot(a, b, dims=((1,), (0,))):
    return lax.dot_general(a, b, (dims, ((), ())), preferred_element_type=F32)


def hidden_rows(rows, w_gate, w_up):
    gate_part = dot(rows, w_gate)
    up_part = dot(rows, w_up)
    return (gate_part / (1.0 + jnp.exp(-gate_part)) * up_part).astype(BF16)


def kernel(
    n, groups, cap,
    tokens_hbm, gain_ref, routes_ref, rw_ref, eg_hbm, eu_hbm, ed_hbm, sg_hbm, su_hbm, sd_hbm,
    out_ref,
    tok, normed, place, scale, wg, wu, wd, fg, fu, fd, sg, su, sd, obuf, arr, ybuf, ret, acc, hid, pick,
    load_sem, wsend, wrecv, xsend, xrecv, dsend, drecv, rsend, rrecv,
):
    half = n // 2
    me = lax.axis_index("ep")
    grp = lax.axis_index("grp")
    base = (me // half) * half
    mine = me % half
    far = (base + half) % n + (mine + half // 2) % half
    rows = tok.shape[0]
    width = tok.shape[1]

    def peer(j):
        total, bit = 0, 1
        while bit < half:
            total = total + bit * (((mine // bit) % 2 + (j // bit) % 2) % 2)
            bit *= 2
        return total

    capp = ret.shape[2]
    if capp > cap:
        low = cap // 16 * 16
        ret[:, :, low:, :] = jnp.zeros((2, half, capp - low, width), BF16)
    barrier = pltpu.get_barrier_semaphore()

    def greet(i, c):
        pl.semaphore_signal(barrier, inc=1, device_id={"ep": base + peer(i)})
        return c

    lax.fori_loop(1, half, greet, 0)
    pl.semaphore_signal(barrier, inc=1, device_id={"ep": far})
    for k in range(1, groups):
        pl.semaphore_signal(barrier, inc=1, device_id={"grp": (grp + k) % groups})

    loads = [(tokens_hbm, tok), (eg_hbm.at[0], wg), (eu_hbm.at[0], wu), (ed_hbm.at[0], wd),
             (sg_hbm, sg), (su_hbm, su), (sd_hbm, sd)]
    loads = [pltpu.make_async_copy(a, b, load_sem.at[i]) for i, (a, b) in enumerate(loads)]
    loads[0].start()

    slab = width // SLABS

    def region(group, a, piece):
        depth = (fg, fu, fd)[a].shape[0] // groups
        if a == 2:
            return pl.ds(pl.multiple_of(group * depth, depth), depth), pl.ds(piece * slab, slab)
        depth = depth // PIECES
        start = (group * PIECES + piece) * depth
        return pl.ds(pl.multiple_of(start, depth), depth), pl.ds(0, fg.shape[1])

    chunks = [(a, piece) for piece in range(PIECES) for a in range(2)]
    chunks += [(2, piece) for piece in range(SLABS)]

    def weight_copy(a, piece):
        src, dst = ((eg_hbm, fg), (eu_hbm, fu), (ed_hbm, fd))[a]
        at, i = region(grp, a, piece), chunks.index((a, piece))
        return pltpu.make_async_remote_copy(
            src_ref=src.at[0, at[0], at[1]], dst_ref=dst.at[at[0], at[1]],
            send_sem=wsend.at[i], recv_sem=wrecv.at[i], device_id={"ep": far})

    def forward_copy(a, piece, k):
        dst = (fg, fu, fd)[a]
        at = region(grp, a, piece)
        i = chunks.index((a, piece)) * max(1, groups - 1) + k - 1
        return pltpu.make_async_remote_copy(
            src_ref=dst.at[at[0], at[1]], dst_ref=dst.at[at[0], at[1]],
            send_sem=xsend.at[i], recv_sem=xrecv.at[i],
            device_id={"grp": (grp + k) % groups})

    pl.semaphore_wait(barrier, half - 1 + 1 + groups - 1)
    weight_copy(*chunks[0]).start()

    lane = lax.broadcasted_iota(jnp.int32, (rows, 128), 1)
    chosen = jnp.zeros((rows, 128), F32)
    weight = jnp.zeros((rows, 128), F32)
    for k in range(routes_ref.shape[1]):
        hit = lane == routes_ref[:, k:k + 1]
        chosen = chosen + jnp.where(hit, 1.0, 0.0)
        weight = weight + jnp.where(hit, rw_ref[:, k:k + 1], 0.0)
    chosen_t = chosen.T
    earlier = (lax.broadcasted_iota(jnp.int32, (rows, rows), 0)
               < lax.broadcasted_iota(jnp.int32, (rows, rows), 1))
    before = dot(chosen_t.astype(BF16), jnp.where(earlier, 1.0, 0.0).astype(BF16))
    place[...] = jnp.where(chosen_t > 0.5, before, -1.0)
    scale[...] = weight.T

    loads[0].wait()
    for copy in loads[1:]:
        copy.start()

    def norm_step(i, c):
        at = pl.ds(pl.multiple_of(i * 32, 32), 32)
        x = tok[at, :].astype(F32)
        factor = lax.rsqrt(jnp.mean(x * x, axis=-1, keepdims=True) + 1e-06)
        normed[at, :] = (x * factor * gain_ref[...]).astype(BF16)
        return c

    lax.fori_loop(0, rows // 32, norm_step, 0)
    slot = lax.broadcasted_iota(jnp.int32, (capp, rows), 0).astype(F32)
    slot = jnp.where(slot < cap, slot, -2.0)

    def gather(p):
        ours = slot == place[pl.ds(base + p, 1), :]
        theirs = slot == place[pl.ds((base + half) % n + (p + half // 2) % half, 1), :]
        want = jnp.concatenate([jnp.where(ours, 1.0, 0.0), jnp.where(theirs, 1.0, 0.0)], axis=0)
        got = dot(want.astype(BF16), normed[...])
        return got[:capp].astype(BF16), got[capp:].astype(BF16)

    used = pl.ds(0, cap)

    def dispatch_copy(p):
        return pltpu.make_async_remote_copy(
            src_ref=obuf.at[:, p, used], dst_ref=arr.at[:, mine, used],
            send_sem=dsend.at[p], recv_sem=drecv.at[mine], device_id={"ep": base + p})

    def dispatch_wait(p):
        pltpu.make_async_remote_copy(
            src_ref=obuf.at[:, p, used], dst_ref=arr.at[:, p, used],
            send_sem=dsend.at[p], recv_sem=drecv.at[p], device_id={"ep": base + p}).wait_recv()

    def message(ref, p, m):
        if m == 0:
            return ref.at[0, p, used]
        return ref.at[1, p, used, pl.ds((m - 1) * slab, slab)]

    def return_copy(p, m):
        return pltpu.make_async_remote_copy(
            src_ref=message(ybuf, p, m), dst_ref=message(ret, mine, m),
            send_sem=rsend.at[p, m], recv_sem=rrecv.at[mine, m], device_id={"ep": base + p})

    def return_wait(p, m):
        pltpu.make_async_remote_copy(
            src_ref=message(ybuf, p, m), dst_ref=message(ret, p, m),
            send_sem=rsend.at[p, m], recv_sem=rrecv.at[p, m],
            device_id={"ep": base + p}).wait_recv()

    def dispatch_step(i, c):
        p = peer(half - 1 - i)
        first, second = gather(p)
        obuf[0, p] = first
        obuf[1, p] = second
        dispatch_copy(p).start()
        return c

    lax.fori_loop(0, half - 1, dispatch_step, 0)
    for a, piece in chunks[1:-SLABS]:
        weight_copy(a, piece).start()
    first, second = gather(mine)
    arr[0, mine] = first
    arr[1, mine] = second

    for copy in loads[4:]:
        copy.wait()
    acc[...] = dot(hidden_rows(normed[...], sg[...], su[...]), sd[...])
    for copy in loads[1:4]:
        copy.wait()

    for b in range(2):
        for p in range(half):
            at = pl.ds((base + b * half) % n + (p + b * (half // 2)) % half, 1)
            want = jnp.where(slot == place[at, :], scale[at, :], 0.0)
            pick[b, p * capp:(p + 1) * capp, :] = want.astype(BF16)

    def own_step(i, c):
        p = peer((i + half // 2 - 1) % (half - 1) + 1)
        dispatch_wait(p)
        ybuf[0, p] = dot(hidden_rows(arr[0, p], wg[...], wu[...]), wd[...]).astype(BF16)
        return_copy(p, 0).start()
        return c

    def forward(a, piece):
        weight_copy(a, piece).wait_recv()
        for k in range(1, groups):
            forward_copy(a, piece, k).start()

    def forwarded(a, piece):
        for k in range(1, groups):
            forward_copy(a, piece, k).wait_recv()

    early = chunks[:-SLABS]
    done = 0
    for i, (a, piece) in enumerate(early):
        until = (half - 1) * (i + 1) // len(early)
        lax.fori_loop(done, until, own_step, 0)
        done = until
        forward(a, piece)
        weight_copy(*chunks[len(early) + i]).start()
    own = dot(hidden_rows(arr[0, mine], wg[...], wu[...]), wd[...]).astype(BF16)
    ret[0, mine] = own

    for a, piece in early:
        forwarded(a, piece)
    hid[...] = hidden_rows(arr[1].reshape(half * capp, width), fg[...], fu[...])

    def far_slab(c):
        forwarded(2, c)
        cols = pl.ds(c * slab, slab)
        got = dot(hid[...], fd[:, cols]).astype(BF16)
        ybuf[1, :, :, cols] = got.reshape(half, capp, slab)

        def send(i, k):
            return_copy(peer(half - 1 - i), 1 + c).start()
            return k

        lax.fori_loop(0, half - 1, send, 0)
        ret[1, mine, :, cols] = ybuf[1, mine, :, cols]

    for c in range(SLABS):
        forward(2, c)
        if c > 0:
            far_slab(c - 1)
    far_slab(SLABS - 1)

    def arrive(m):
        def step(i, k):
            return_wait(peer(i + 1), m)
            return k

        lax.fori_loop(0, half - 1, step, 0)

    arrive(0)
    acc[...] += dot(pick[0], ret[0].reshape(half * capp, width), ((0,), (0,)))
    for c in range(SLABS):
        arrive(1 + c)
        cols = pl.ds(c * slab, slab)
        total = acc[:, cols] + dot(
            pick[1], ret[1, :, :, cols].reshape(half * capp, slab), ((0,), (0,)))
        out_ref[:, cols] = total.astype(BF16)

    def drain(i, c):
        p = peer(half - 1 - i)
        dispatch_copy(p).wait_send()
        for m in range(1 + SLABS):
            return_copy(p, m).wait_send()
        return c

    lax.fori_loop(0, half - 1, drain, 0)
    for a, piece in chunks:
        weight_copy(a, piece).wait_send()
        for k in range(1, groups):
            forward_copy(a, piece, k).wait_send()


def on_device(tokens, norm_gain, routes, route_weights, expert_gate, expert_up, expert_down,
              shared_gate, shared_up, shared_down):
    rows, width = tokens.shape
    n, groups = lax.axis_size("ep"), lax.axis_size("grp")
    half = n // 2
    cap = -(-(5 * rows * routes.shape[1] // (4 * n)) // 8) * 8
    nchunk = 2 * PIECES + SLABS
    nfwd = nchunk * max(1, groups - 1)
    vmem = lambda shape, kind=BF16: pltpu.VMEM(shape, kind)
    anyspec = pl.BlockSpec(memory_space=pl.ANY)
    vspec = pl.BlockSpec(memory_space=pltpu.VMEM)
    capp = cap
    block = (2, half, capp, width)
    return pl.pallas_call(
        functools.partial(kernel, n, groups, cap),
        out_shape=jax.ShapeDtypeStruct((rows, width), BF16),
        in_specs=[anyspec, vspec, vspec, vspec] + [anyspec] * 6,
        out_specs=vspec,
        scratch_shapes=[
            vmem((rows, width)), vmem((rows, width)), vmem((128, rows), F32), vmem((128, rows), F32),
            vmem(expert_gate.shape[1:]), vmem(expert_up.shape[1:]), vmem(expert_down.shape[1:]),
            vmem(expert_gate.shape[1:]), vmem(expert_up.shape[1:]), vmem(expert_down.shape[1:]),
            vmem(shared_gate.shape), vmem(shared_up.shape), vmem(shared_down.shape),
            vmem(block), vmem(block), vmem(block), vmem(block), vmem((rows, width), F32),
            vmem((half * capp, expert_gate.shape[2])), vmem((2, half * capp, rows)),
            pltpu.SemaphoreType.DMA((7,)),
            pltpu.SemaphoreType.DMA((nchunk,)), pltpu.SemaphoreType.DMA((nchunk,)),
            pltpu.SemaphoreType.DMA((nfwd,)), pltpu.SemaphoreType.DMA((nfwd,)),
            pltpu.SemaphoreType.DMA((half,)), pltpu.SemaphoreType.DMA((half,)),
            pltpu.SemaphoreType.DMA((half, 1 + SLABS)), pltpu.SemaphoreType.DMA((half, 1 + SLABS)),
        ],
        compiler_params=pltpu.CompilerParams(
            collective_id=0, has_side_effects=True, vmem_limit_bytes=60 * 1024 * 1024),
    )(tokens, norm_gain.reshape(1, width), routes, route_weights, expert_gate, expert_up,
      expert_down, shared_gate, shared_up, shared_down)


def solution(mesh):
    return jax.shard_map(
        on_device,
        mesh=mesh,
        in_specs=(
            P(("grp", "ep"), None),
            P(),
            P(("grp", "ep"), None),
            P(("grp", "ep"), None),
            P("ep", None, None),
            P("ep", None, None),
            P("ep", None, None),
            P(),
            P(),
            P(),
        ),
        out_specs=P(("grp", "ep"), None),
        check_vma=False,
    )
```
